32 devices in a mesh: ep: 8 (over z, y), tp: 4 (over x, core).
Axes of the slice: x: 2, y: 2, z: 4, core: 2. Of those that a mesh axis runs over, the one named last changes fastest.
Arguments:
- mixer_in: bfloat16 [8192, 4096], P('ep', 'tp'), may hold values from -110 to 110
- mixer_gain: float32 [4096], P('tp'), may hold values from 0.1 to 1.9
- pool_weight: bfloat16 [4, 1024, 1024], P('tp'), may hold values from -0.1875 to 0.1875
- pool_scale: float32 [4096], P('tp'), may hold values from 0.1 to 1.9
- moe_in: bfloat16 [2048, 4096], P('ep'), may hold values from -6 to 6
- moe_gain: float32 [4096], replicated, may hold values from 0.1 to 1.9
- route_expert: int32 [2048, 2], P('ep'), may hold values from 0 to 7, as said below
- route_weight: float32 [2048, 2], P('ep'), may hold values from 0.1 to 1
- gate_weight: bfloat16 [8, 4096, 1024], P('ep', None, 'tp'), may hold values from -0.09375 to 0.09375
- up_weight: bfloat16 [8, 4096, 1024], P('ep', None, 'tp'), may hold values from -0.09375 to 0.09375
- down_weight: bfloat16 [8, 1024, 4096], P('ep', 'tp'), may hold values from -0.1875 to 0.1875
Outputs:
- mixer_out: bfloat16 [8192, 4096], P('ep', 'tp')
- moe_out: bfloat16 [2048, 4096], P('ep', 'tp')
The draws below stay inside these ranges and needn't reach their ends.
Inputs may be any that keep to these rules, and one draw needn't show every extreme that they name: `route_expert`: both experts of a row are different and lie in one group: the group of an expert is its number divided by 2, rounded down. Among the rows of one index of ep no expert is named more than 96 times; in every draw the experts of some group are each named exactly 96 times by the rows of every index of ep.
All inputs are finite; a program needn't handle non-finite values.
Results may differ from the reference program's by a relative error of at most 0.0071.
Values may be sent and summed in bfloat16 or wider, within the bound.
No kernel may reach another device: no remote copies, remote signals or barrier semaphores. Data moves between devices by JAX's collectives and lax.ppermute only.
A program may use at most 128 MiB of HBM per device.

```python
import math
import jax
import jax.numpy as jnp
from jax import lax

D = 4096
POOL_GROUPS = 4
CH = 1024
WINDOW_MAX = 16
FF = 1024
EXPERTS = 8
EXPERT_GROUPS = 4
GROUP_EXPERTS = 2
MOE_DEV = 256
CAP = 96
TOKENS_A = 8192
TOKENS_B = 2048
N_EP = 8


def draw_mixer_in(key, part):
    first, second = jax.random.split(key, 2)
    ramp = jnp.exp(jnp.log(4.0) * jnp.arange(D, dtype=jnp.float32) / D)
    ramp = ramp * jnp.exp(jax.random.uniform(second, (D,), jnp.float32, -0.35, 0.35))
    base = jax.random.truncated_normal(first, -6.0, 6.0, (TOKENS_A, D), jnp.float32)
    return (base * ramp[None, :]).astype(jnp.bfloat16)


def draw_route_expert(key, part):
    fullest = GROUP_EXPERTS * CAP // 2
    rest = MOE_DEV - fullest
    pick_key, block_key = jax.random.split(key, 2)
    full_group = jax.random.randint(pick_key, (), 0, EXPERT_GROUPS)

    def one_block(bkey):
        key_a, key_b, key_c, key_d = jax.random.split(bkey, 4)
        chosen = jax.random.permutation(key_a, (EXPERT_GROUPS - 1) * fullest)[:rest]
        other_group = (full_group + 1 + chosen // fullest) % EXPERT_GROUPS
        groups = jnp.concatenate([jnp.full((fullest,), full_group, jnp.int32), other_group.astype(jnp.int32)])
        ranks = jnp.concatenate([jnp.arange(fullest, dtype=jnp.int32), (chosen % fullest).astype(jnp.int32)])
        shifts = jax.random.randint(key_b, (EXPERT_GROUPS,), 1, GROUP_EXPERTS)
        labels = jax.vmap(lambda lkey: jax.random.permutation(lkey, GROUP_EXPERTS))(jax.random.split(key_c, EXPERT_GROUPS))
        first = labels[groups, ranks % GROUP_EXPERTS]
        second = labels[groups, (ranks + shifts[groups]) % GROUP_EXPERTS]
        pair = jnp.stack([first, second], axis=1) + groups[:, None] * GROUP_EXPERTS
        order = jax.random.permutation(key_d, MOE_DEV)
        return pair[order].astype(jnp.int32)
    blocks = jax.vmap(one_block)(jax.random.split(block_key, N_EP))
    return blocks.reshape(MOE_DEV * N_EP, 2)


def steps_of(own_key, extent, cuts, least, largest):
    def one(axis_at, shards_of):
        steps = jax.random.uniform(jax.random.fold_in(jax.random.fold_in(own_key, 6), axis_at), (shards_of,), jnp.float32, least / len(cuts), largest / len(cuts))
        return jnp.repeat(jnp.exp(steps), extent[axis_at] // shards_of).reshape((-1,) + (1,) * (len(extent) - axis_at - 1))

    level = one(*cuts[0])
    for cut in cuts[1:]:
        level = level * one(*cut)
    return level


def bell_draw(own_key, dims, deviation, bound, pieces=(), kind=jnp.bfloat16):
    drawn = deviation * jax.random.normal(own_key, dims, jnp.float32)
    if pieces:
        drawn = drawn * steps_of(own_key, dims, pieces, -0.22, 0.18)
    return jnp.clip(drawn, -bound, bound).astype(kind)


def setup_inputs(seed: int = 0) -> dict:
    seeds = jax.random.split(jax.random.key(seed), 12)
    return {
        "mixer_in": draw_mixer_in(jax.random.fold_in(seeds[11], 71), 0),
        "mixer_gain": jnp.clip(1.0 + 0.18 * jax.random.normal(seeds[1], (D,), jnp.float32), 0.1, 1.9),
        "pool_weight": bell_draw(seeds[2], (POOL_GROUPS, CH, CH), CH ** -0.5, 0.1875, ((0, 4),)),
        "pool_scale": jnp.clip(1.0 + 0.18 * jax.random.normal(seeds[3], (D,), jnp.float32), 0.1, 1.9),
        "moe_in": bell_draw(seeds[4], (TOKENS_B, D), 1.0, 6.0, ((0, 8),)),
        "moe_gain": jnp.clip(1.0 + 0.18 * jax.random.normal(seeds[5], (D,), jnp.float32), 0.1, 1.9),
        "route_expert": draw_route_expert(jax.random.fold_in(seeds[11], 71), 0),
        "route_weight": jnp.clip(jnp.exp(math.log(1.0) - 2.3025851 * jax.random.uniform(seeds[7], (TOKENS_B, 2), jnp.float32) ** steps_of(seeds[7], (TOKENS_B, 2), ((0, 8),), -0.2, 0.2)), 0.1, 1.0),
        "gate_weight": bell_draw(seeds[8], (EXPERTS, D, FF), D ** -0.5, 0.09375, ((0, 8), (2, 4))),
        "up_weight": bell_draw(seeds[9], (EXPERTS, D, FF), D ** -0.5, 0.09375, ((0, 8), (2, 4))),
        "down_weight": bell_draw(seeds[10], (EXPERTS, FF, D), FF ** -0.5, 0.1875, ((0, 8), (1, 4))),
    }


EPS = 1e-06

def reference(mixer_in, mixer_gain, pool_weight, pool_scale, moe_in, moe_gain, route_expert, route_weight, gate_weight, up_weight, down_weight):
    feats = mixer_in.astype(jnp.float32)
    normed_a = (feats * lax.rsqrt(lax.optimization_barrier(jnp.mean(feats * feats, axis=1, keepdims=True)) + EPS) * mixer_gain).astype(jnp.bfloat16)
    reach = WINDOW_MAX - 1
    position = jnp.arange(TOKENS_A, dtype=jnp.int32)
    outputs = []
    for group in range(POOL_GROUPS):
        span = 2 ** (group + 1)
        block = normed_a[:, group * CH:(group + 1) * CH].astype(jnp.float32)
        padded = jnp.pad(block, ((reach, 0), (0, 0)))
        running = jnp.zeros_like(block)
        for offset in range(span):
            running = running + padded[reach - offset:reach - offset + TOKENS_A]
        count = jnp.minimum(position + 1, span).astype(jnp.float32)[:, None]
        pooled = (running / count - block).astype(jnp.bfloat16)
        projected = jnp.dot(pooled, pool_weight[group], preferred_element_type=jnp.float32)
        outputs.append(projected * pool_scale[group * CH:(group + 1) * CH])
    mixer_out = jnp.concatenate(outputs, axis=1).astype(jnp.bfloat16)
    feats_b = moe_in.astype(jnp.float32)
    normed_b = (feats_b * lax.rsqrt(lax.optimization_barrier(jnp.mean(feats_b * feats_b, axis=1, keepdims=True)) + EPS) * moe_gain).astype(jnp.bfloat16)
    slots_all = N_EP * CAP
    flat = route_expert.reshape(-1).astype(jnp.int32)
    onehot = (flat[:, None] == jnp.arange(EXPERTS, dtype=jnp.int32)[None, :]).astype(jnp.int32)
    earlier = jnp.cumsum(onehot, axis=0) - onehot
    slot_pos = lax.optimization_barrier(jnp.sum(earlier * onehot, axis=1)).astype(jnp.int32)
    owner = (jnp.arange(2 * TOKENS_B, dtype=jnp.int32) // 2).astype(jnp.int32)
    table = jnp.full((EXPERTS, slots_all), TOKENS_B, jnp.int32).at[flat, slot_pos].set(owner)
    padded_b = jnp.concatenate([normed_b, jnp.zeros((1, D), jnp.bfloat16)], axis=0)

    def one_expert(items):
        index, w_gate, w_up, w_down = items
        rows = jnp.take(padded_b, index, axis=0)
        gate = jnp.dot(rows, w_gate, preferred_element_type=jnp.float32)
        upper = jnp.dot(rows, w_up, preferred_element_type=jnp.float32)
        hidden = (jax.nn.silu(gate) * upper).astype(jnp.bfloat16)
        return jnp.dot(hidden, w_down, preferred_element_type=jnp.float32).astype(jnp.bfloat16)
    results = lax.map(one_expert, (table, gate_weight, up_weight, down_weight))
    picked = jnp.take(results.reshape(EXPERTS * slots_all, D), flat * slots_all + slot_pos, axis=0)
    weighted = picked.astype(jnp.float32).reshape(TOKENS_B, 2, D) * route_weight[:, :, None]
    moe_out = lax.optimization_barrier(jnp.sum(weighted, axis=1)).astype(jnp.bfloat16)
    return (mixer_out, moe_out)
```

```python
import jax
import jax.numpy as jnp
from jax import lax
from jax.experimental import pallas as pl
from jax.experimental.pallas import tpu as pltpu
from jax.sharding import Mesh, PartitionSpec as P

D = 4096
WINDOW_MAX = 16
EXPERT_GROUPS = 4


EPS = 1e-06


def passed_along(value, axis, steps):
    count = lax.axis_size(axis)
    first, last = (max(0, -steps), min(count, count - steps))
    return lax.ppermute(value, axis, [(source, source + steps) for source in range(first, last)])


def shards(
    mixer_in,
    mixer_gain,
    pool_weight,
    pool_scale,
    moe_in,
    moe_gain,
    route_expert,
    route_weight,
    gate_weight,
    up_weight,
    down_weight,
):
    rows = mixer_in.shape[0]
    feats = mixer_in.astype(jnp.float32)
    squares = lax.psum(jnp.sum(feats * feats, axis=1), "tp")
    normed_a = (feats * lax.rsqrt(squares[:, None] / D + EPS) * mixer_gain).astype(jnp.bfloat16)
    reach = WINDOW_MAX - 1
    before = passed_along(normed_a[rows - reach :], "ep", 1)
    extended = jnp.concatenate([before, normed_a], axis=0).astype(jnp.float32)
    running = jnp.zeros((rows, normed_a.shape[1]), jnp.float32)
    totals = []
    for offset in range(WINDOW_MAX):
        running = running + lax.slice_in_dim(
            extended, reach - offset, reach - offset + rows, axis=0
        )
        if offset > 0 and offset + 1 & offset == 0:
            totals.append(running)
    group = lax.axis_index("tp")
    window_sum = lax.dynamic_index_in_dim(jnp.stack(totals), group, 0, keepdims=False)
    span = jnp.left_shift(jnp.int32(2), group)
    position = lax.axis_index("ep") * rows + jnp.arange(rows, dtype=jnp.int32)
    count = jnp.minimum(position + 1, span).astype(jnp.float32)[:, None]
    pooled = (window_sum / count - extended[reach:]).astype(jnp.bfloat16)
    mixer_out = (
        jnp.dot(pooled, pool_weight[0], preferred_element_type=jnp.float32) * pool_scale
    ).astype(jnp.bfloat16)
    tokens = moe_in.shape[0]
    feats_b = moe_in.astype(jnp.float32)
    normed_b = (
        feats_b * lax.rsqrt(jnp.mean(feats_b * feats_b, axis=1, keepdims=True) + EPS) * moe_gain
    ).astype(jnp.bfloat16)
    experts = gate_weight.shape[0] * lax.axis_size("ep")
    slots = 3 * tokens // experts
    flat = route_expert.reshape(-1)
    onehot = (flat[:, None] == jnp.arange(experts, dtype=jnp.int32)[None, :]).astype(jnp.int32)
    earlier = jnp.cumsum(onehot, axis=0) - onehot
    slot_index = flat * slots + jnp.sum(earlier * onehot, axis=1)
    owner = jnp.arange(2 * tokens, dtype=jnp.int32) // 2
    source = jnp.full((experts * slots,), tokens, jnp.int32).at[slot_index].set(owner)
    padded_b = jnp.concatenate([normed_b, jnp.zeros((1, D), jnp.bfloat16)], axis=0)
    outgoing = jnp.take(padded_b, source, axis=0).reshape(experts, slots, D)
    w_gate = gate_weight[0]
    w_up = up_weight[0]
    share = slots // lax.axis_size("tp")
    mine = lax.dynamic_slice_in_dim(outgoing, lax.axis_index("tp") * share, share, 1)
    arrived = lax.all_to_all(mine, "ep", split_axis=0, concat_axis=0, tiled=True)
    expand_arrived = lax.all_gather(arrived, "tp", axis=1, tiled=True)
    gate = jnp.einsum("nkd,df->nkf", expand_arrived, w_gate, preferred_element_type=jnp.float32)
    upper = jnp.einsum("nkd,df->nkf", expand_arrived, w_up, preferred_element_type=jnp.float32)
    hidden = (jax.nn.silu(gate) * upper).astype(jnp.bfloat16)
    flat_hidden = hidden.reshape(-1, hidden.shape[2])
    w_down = down_weight[0]
    columns = D // lax.axis_size("tp")
    summed = lax.psum_scatter(
        lax.dot_general(
            w_down, flat_hidden, (((0,), (1,)), ((), ())), preferred_element_type=jnp.float32
        ),
        "tp",
        scatter_dimension=0,
        tiled=True,
    ).astype(jnp.bfloat16)
    back = lax.all_to_all(
        summed.reshape(columns, -1, slots), "ep", split_axis=1, concat_axis=1, tiled=True
    )
    picked = jnp.take(back.reshape(columns, experts * slots), slot_index, axis=1)
    weighted = picked.astype(jnp.float32).reshape(columns, tokens, 2) * route_weight[None, :, :]
    moe_out = jnp.sum(weighted, axis=2).T.astype(jnp.bfloat16)
    return (mixer_out, moe_out)


F32, BF16, I32 = jnp.float32, jnp.bfloat16, jnp.int32
EXTRA = 128


def swapped(value, axis):
    return lax.ppermute(value, axis, [(i, i ^ 1) for i in range(lax.axis_size(axis))])


def turned(value, axis, steps):
    count = lax.axis_size(axis)
    return lax.ppermute(value, axis, [(i, (i + steps) % count) for i in range(count)])


def vmem():
    return pl.BlockSpec(memory_space=pltpu.VMEM)


def smem():
    return pl.BlockSpec(memory_space=pltpu.SMEM)


def dot(a, b):
    return jnp.dot(a, b, preferred_element_type=F32)


def dispatch(moe_in, moe_gain, expert_rows, weight_rows, place, cap):
    tokens, width = moe_in.shape
    half = cap // 2
    groups = EXPERT_GROUPS

    def kernel(place_ref, x_ref, gain_ref, expert_ref, weight_ref, key_ref, *out_refs):
        x = x_ref[...].astype(F32)
        scale = lax.rsqrt(jnp.sum(x * x, axis=1, keepdims=True) / width + EPS)
        normed = (x * scale * gain_ref[...]).astype(BF16)
        z, c = place_ref[0], place_ref[1]
        expert = expert_ref[...]
        first = expert[0:1]
        group = lax.shift_right_logical(first, 1)
        member = (lax.broadcasted_iota(I32, (8, tokens), 0) == group).astype(F32)
        before = lax.broadcasted_iota(I32, (tokens, tokens), 0) < lax.broadcasted_iota(
            I32, (tokens, tokens), 1
        )
        earlier = dot(member.astype(BF16), before.astype(BF16))
        slot = jnp.sum(member * earlier, axis=0, keepdims=True).astype(I32)
        ahead = group - z
        ahead = jnp.where(ahead < 0, ahead + groups, ahead)
        local = slot - c * half
        mine = (local >= 0) & (local < half)
        local = jnp.where(local < 0, local + cap, local)
        key_ref[...] = jnp.broadcast_to(ahead * cap + local, (8, tokens))
        sent = jnp.where(mine, ahead * half + local, -1)
        pick = (lax.broadcasted_iota(I32, (groups * half, tokens), 0) == sent).astype(BF16)
        weight = weight_ref[...]
        even = (first & 1) == 0
        low = jnp.where(even, weight[0:1], weight[1:2])
        high = jnp.where(even, weight[1:2], weight[0:1])
        parts = []
        for w in (low, high):
            top = w.astype(BF16)
            parts += [top, (w - top.astype(F32)).astype(BF16)]
        lane = lax.broadcasted_iota(I32, (8, EXTRA), 1)
        row = lax.broadcasted_iota(I32, (8, EXTRA), 0)
        spread = (lane == row).astype(BF16)
        stacked = jnp.concatenate(
            [p.astype(F32) for p in parts] + [jnp.zeros((4, tokens), F32)], axis=0
        ).astype(BF16)
        table = lax.dot_general(
            stacked, spread, (((0,), (0,)), ((), ())), preferred_element_type=F32
        ).astype(BF16)
        rows = dot(pick, normed).astype(BF16)
        extra = dot(pick, table).astype(BF16)
        for d in range(groups):
            out_refs[d][:, :width] = rows[d * half : (d + 1) * half]
            out_refs[d][:, width:] = extra[d * half : (d + 1) * half]

    return pl.pallas_call(
        kernel,
        out_shape=[jax.ShapeDtypeStruct((8, tokens), I32)]
        + [jax.ShapeDtypeStruct((half, width + EXTRA), BF16)] * groups,
        in_specs=[smem(), vmem(), vmem(), vmem(), vmem()],
        out_specs=[vmem()] * (1 + groups),
        name="dispatch",
    )(place, moe_in, moe_gain.reshape(1, width), expert_rows, weight_rows)


def expand(pieces, w_gate, w_up, pair):
    width, units = w_gate.shape
    step = 512
    steps = width // step
    total = sum(p.shape[0] for p in pieces)
    count = len(pieces)

    def kernel(pair_ref, *refs):
        xs, extras = refs[:count], refs[count : 2 * count]
        gate_ref, up_ref, out_ref, gate_sum, up_sum = refs[2 * count :]
        k = pl.program_id(0)

        @pl.when(k == 0)
        def _():
            gate_sum[...] = jnp.zeros_like(gate_sum)
            up_sum[...] = jnp.zeros_like(up_sum)

        x = jnp.concatenate([r[...] for r in xs], axis=0)
        gate_sum[...] += dot(x, gate_ref[...])
        up_sum[...] += dot(x, up_ref[...])

        @pl.when(k == steps - 1)
        def _():
            extra = jnp.concatenate([r[...] for r in extras], axis=0).astype(F32)
            lane = lax.broadcasted_iota(I32, extra.shape, 1)
            wanted = lax.shift_right_logical(lane, 1) == pair_ref[0]
            weight = jnp.sum(jnp.where(wanted, extra, 0.0), axis=1, keepdims=True)
            gate = gate_sum[...]
            out_ref[...] = (gate / (1.0 + jnp.exp(-gate)) * up_sum[...] * weight).astype(BF16)

    return pl.pallas_call(
        kernel,
        grid=(steps,),
        out_shape=jax.ShapeDtypeStruct((total, units), BF16),
        in_specs=[smem()]
        + [pl.BlockSpec((p.shape[0], step), lambda k: (0, k)) for p in pieces]
        + [pl.BlockSpec((p.shape[0], EXTRA), lambda k: (0, width // EXTRA)) for p in pieces]
        + [pl.BlockSpec((step, units), lambda k: (k, 0))] * 2,
        out_specs=pl.BlockSpec((total, units), lambda k: (0, 0)),
        scratch_shapes=[pltpu.VMEM((total, units), F32)] * 2,
        name="expand",
    )(pair, *pieces, *pieces, w_gate, w_up)


def contract(own, beside, across, w_own, w_beside, w_across, runs):
    units = own.shape[1]
    columns = w_own.shape[1]
    kept = sum(n for _, n, other, _ in runs if not other)
    total = own.shape[0]

    def kernel(own_ref, beside_ref, across_ref, wo_ref, wb_ref, wa_ref, keep_ref, send_ref):
        near = [s for s, _, _, far in runs if not far]
        far = [s for s, _, _, far in runs if far]
        partner = dict(zip(near + far, far + near))
        swapped_rows = jnp.concatenate(
            [across_ref[partner[s] : partner[s] + n] for s, n, _, _ in runs], axis=0
        )
        out = dot(own_ref[...], wo_ref[...])
        out = out + dot(beside_ref[...], wb_ref[...])
        out = out + dot(swapped_rows, wa_ref[...])
        out = out.astype(BF16)
        at = {False: 0, True: 0}
        for s, n, other, _ in runs:
            ref = send_ref if other else keep_ref
            ref[at[other] : at[other] + n] = out[s : s + n]
            at[other] += n

    return pl.pallas_call(
        kernel,
        out_shape=[
            jax.ShapeDtypeStruct((kept, columns), BF16),
            jax.ShapeDtypeStruct((total - kept, columns), BF16),
        ],
        in_specs=[vmem()] * 6,
        out_specs=[vmem()] * 2,
        name="contract",
    )(own, beside, across, w_own, w_beside, w_across)


def restore(key, pieces):
    tokens = key.shape[1]
    cap, columns = pieces[0].shape

    def kernel(key_ref, *refs):
        out_ref = refs[-1]
        total = None
        for d, r in enumerate(refs[:-1]):
            row = lax.broadcasted_iota(I32, (cap, tokens), 0) + d * cap
            pick = (row == key_ref[0:1]).astype(BF16)
            part = lax.dot_general(
                pick, r[...], (((0,), (0,)), ((), ())), preferred_element_type=F32
            )
            total = part if total is None else total + part
        out_ref[...] = total.astype(BF16)

    return pl.pallas_call(
        kernel,
        out_shape=jax.ShapeDtypeStruct((tokens, columns), BF16),
        in_specs=[vmem()] * (1 + len(pieces)),
        out_specs=vmem(),
        name="restore",
    )(key, *pieces)


def pool(mixer_in, halo, squares, gain, weight, scale, place):
    rows, width = mixer_in.shape
    reach = WINDOW_MAX
    block = 256
    steps = rows // block

    def kernel(place_ref, x_ref, prev_ref, halo_ref, sq_ref, psq_ref, gain_ref, w_ref, s_ref, out_ref):
        i = pl.program_id(0)
        span = lax.shift_left(jnp.int32(2), place_ref[1])
        ahead = jnp.where(i == 0, halo_ref[...].astype(F32), prev_ref[...].astype(F32))
        x = jnp.concatenate([ahead, x_ref[...].astype(F32)], axis=0)
        total = jnp.concatenate([psq_ref[...], sq_ref[...]], axis=0)
        normed = (x * lax.rsqrt(total / D + EPS) * gain_ref[...]).astype(BF16)
        r = lax.broadcasted_iota(I32, (block, block + reach), 0)
        q = lax.broadcasted_iota(I32, (block, block + reach), 1)
        back = r + reach - q
        band = ((back >= 0) & (back < span)).astype(BF16)
        sums = dot(band, normed)
        position = place_ref[0] * rows + i * block + lax.broadcasted_iota(I32, (block, 1), 0)
        count = jnp.minimum(position + 1, span).astype(F32)
        pooled = (sums / count - normed[reach:].astype(F32)).astype(BF16)
        out_ref[...] = (dot(pooled, w_ref[...]) * s_ref[...]).astype(BF16)

    ratio = block // reach
    return pl.pallas_call(
        kernel,
        grid=(steps,),
        out_shape=jax.ShapeDtypeStruct((rows, width), BF16),
        in_specs=[
            smem(),
            pl.BlockSpec((block, width), lambda i: (i, 0)),
            pl.BlockSpec((reach, width), lambda i: (jnp.maximum(i * ratio - 1, 0), 0)),
            pl.BlockSpec((reach, width), lambda i: (0, 0)),
            pl.BlockSpec((block, 1), lambda i: (i, 0)),
            pl.BlockSpec((reach, 1), lambda i: (jnp.where(i == 0, steps * ratio, i * ratio - 1), 0)),
            pl.BlockSpec((1, width), lambda i: (0, 0)),
            pl.BlockSpec((width, width), lambda i: (0, 0)),
            pl.BlockSpec((1, width), lambda i: (0, 0)),
        ],
        out_specs=pl.BlockSpec((block, width), lambda i: (i, 0)),
        name="pool",
    )(
        place,
        mixer_in,
        mixer_in,
        halo,
        squares,
        squares,
        gain.reshape(1, width),
        weight,
        scale.reshape(1, width),
    )


def paired(
    mixer_in,
    mixer_gain,
    pool_weight,
    pool_scale,
    moe_in,
    moe_gain,
    route_expert,
    route_weight,
    gate_weight,
    up_weight,
    down_weight,
):
    z, y, x, c = (lax.axis_index(a) for a in ("z", "y", "x", "c"))
    tokens = moe_in.shape[0]
    cap = 3 * tokens // (2 * EXPERT_GROUPS)
    half = cap // 2

    key, *sends = dispatch(
        moe_in, moe_gain, route_expert.T, route_weight.T, jnp.stack([z, c]).astype(I32), cap
    )
    come = [sends[0], turned(sends[1], "z", 1), turned(sends[2], "z", 2), turned(sends[3], "z", 3)]
    other = [swapped(v, "y") for v in come]
    w_gate, w_up, w_down = gate_weight[0], up_weight[0], down_weight[0]

    quarter = w_down.shape[1] // (2 * lax.axis_size("x"))
    away = lax.dynamic_slice_in_dim(w_down, (1 - x) * 2 * quarter, 2 * quarter, 1)
    w_beside2 = swapped(away, "x")
    mine_at, twin_at = (2 * x + c) * quarter, (2 * x + 1 - c) * quarter
    w_own = lax.dynamic_slice_in_dim(w_down, mine_at, quarter, 1)
    w_beside = lax.dynamic_slice_in_dim(w_beside2, c * quarter, quarter, 1)
    w_across = swapped(
        jnp.concatenate(
            [
                lax.dynamic_slice_in_dim(w_down, twin_at, quarter, 1),
                lax.dynamic_slice_in_dim(w_beside2, (1 - c) * quarter, quarter, 1),
            ],
            axis=0,
        ),
        "c",
    )

    pair = y.astype(I32).reshape(1)
    results = [None] * EXPERT_GROUPS
    for chunk in ((0, 1, 3), (2,)):
        near = [v for d in chunk for v in (come[d], other[d])]
        far = [swapped(v, "c") for v in near]
        hidden = expand(near + far, w_gate, w_up, pair)
        beside = swapped(hidden, "x")
        across = swapped(jnp.concatenate([hidden, beside], axis=1), "c")
        runs = []
        for is_far in (False, True):
            for d in chunk:
                for is_other in (False, True):
                    runs.append((len(runs) * half, half, is_other, is_far))
        keep, send = contract(hidden, beside, across, w_own, w_beside, w_across, runs)
        got = swapped(send, "y")
        both = (keep.astype(F32) + got.astype(F32)).astype(BF16)
        n = len(chunk)
        for at, d in enumerate(chunk):
            rows = jnp.concatenate(
                [both[at * half : (at + 1) * half], both[(n + at) * half : (n + at + 1) * half]], axis=0
            )
            results[d] = turned(rows, "z", -d) if d else rows
    moe_out = restore(key, results)

    rows = mixer_in.shape[0]
    reach = WINDOW_MAX
    halo = passed_along(mixer_in[rows - reach :], ("z", "y"), 1)
    squares = jnp.concatenate(
        [jnp.sum(jnp.square(v.astype(F32)), axis=1) for v in (mixer_in, halo)]
    )
    squares = squares + swapped(squares, "c")
    squares = squares + swapped(squares, "x")
    place = jnp.stack([z * lax.axis_size("y") + y, 2 * x + c]).astype(I32)
    mixer_out = pool(
        mixer_in, halo, squares[:, None], mixer_gain, pool_weight[0], pool_scale, place
    )
    return (mixer_out, moe_out)


def solution(mesh):
    ep, tp = mesh.shape["ep"], mesh.shape["tp"]
    body, over, a, b = shards, mesh, "ep", "tp"
    if ep == 2 * EXPERT_GROUPS and tp == 4:
        shape = (EXPERT_GROUPS, 2, 2, 2)
        over = Mesh(mesh.devices.reshape(shape), ("z", "y", "x", "c"))
        body, a, b = paired, ("z", "y"), ("x", "c")
    return jax.shard_map(
        body,
        mesh=over,
        in_specs=(
            P(a, b),
            P(b),
            P(b, None, None),
            P(b),
            P(a, None),
            P(),
            P(a, None),
            P(a, None),
            P(a, None, b),
            P(a, None, b),
            P(a, b, None),
        ),
        out_specs=(P(a, b), P(a, b)),
        check_vma=False,
    )
```

```python
import jax
import jax.numpy as jnp
from jax import lax
from jax.experimental import pallas as pl
from jax.experimental.pallas import tpu as pltpu
from jax.sharding import Mesh, PartitionSpec as P

D = 4096
WINDOW_MAX = 16
EXPERT_GROUPS = 4


EPS = 1e-06


def passed_along(value, axis, steps):
    count = lax.axis_size(axis)
    first, last = (max(0, -steps), min(count, count - steps))
    return lax.ppermute(value, axis, [(source, source + steps) for source in range(first, last)])


def shards(
    mixer_in,
    mixer_gain,
    pool_weight,
    pool_scale,
    moe_in,
    moe_gain,
    route_expert,
    route_weight,
    gate_weight,
    up_weight,
    down_weight,
):
    rows = mixer_in.shape[0]
    feats = mixer_in.astype(jnp.float32)
    squares = lax.psum(jnp.sum(feats * feats, axis=1), "tp")
    normed_a = (feats * lax.rsqrt(squares[:, None] / D + EPS) * mixer_gain).astype(jnp.bfloat16)
    reach = WINDOW_MAX - 1
    before = passed_along(normed_a[rows - reach :], "ep", 1)
    extended = jnp.concatenate([before, normed_a], axis=0).astype(jnp.float32)
    running = jnp.zeros((rows, normed_a.shape[1]), jnp.float32)
    totals = []
    for offset in range(WINDOW_MAX):
        running = running + lax.slice_in_dim(
            extended, reach - offset, reach - offset + rows, axis=0
        )
        if offset > 0 and offset + 1 & offset == 0:
            totals.append(running)
    group = lax.axis_index("tp")
    window_sum = lax.dynamic_index_in_dim(jnp.stack(totals), group, 0, keepdims=False)
    span = jnp.left_shift(jnp.int32(2), group)
    position = lax.axis_index("ep") * rows + jnp.arange(rows, dtype=jnp.int32)
    count = jnp.minimum(position + 1, span).astype(jnp.float32)[:, None]
    pooled = (window_sum / count - extended[reach:]).astype(jnp.bfloat16)
    mixer_out = (
        jnp.dot(pooled, pool_weight[0], preferred_element_type=jnp.float32) * pool_scale
    ).astype(jnp.bfloat16)
    tokens = moe_in.shape[0]
    feats_b = moe_in.astype(jnp.float32)
    normed_b = (
        feats_b * lax.rsqrt(jnp.mean(feats_b * feats_b, axis=1, keepdims=True) + EPS) * moe_gain
    ).astype(jnp.bfloat16)
    experts = gate_weight.shape[0] * lax.axis_size("ep")
    slots = 3 * tokens // experts
    flat = route_expert.reshape(-1)
    onehot = (flat[:, None] == jnp.arange(experts, dtype=jnp.int32)[None, :]).astype(jnp.int32)
    earlier = jnp.cumsum(onehot, axis=0) - onehot
    slot_index = flat * slots + jnp.sum(earlier * onehot, axis=1)
    owner = jnp.arange(2 * tokens, dtype=jnp.int32) // 2
    source = jnp.full((experts * slots,), tokens, jnp.int32).at[slot_index].set(owner)
    padded_b = jnp.concatenate([normed_b, jnp.zeros((1, D), jnp.bfloat16)], axis=0)
    outgoing = jnp.take(padded_b, source, axis=0).reshape(experts, slots, D)
    w_gate = gate_weight[0]
    w_up = up_weight[0]
    share = slots // lax.axis_size("tp")
    mine = lax.dynamic_slice_in_dim(outgoing, lax.axis_index("tp") * share, share, 1)
    arrived = lax.all_to_all(mine, "ep", split_axis=0, concat_axis=0, tiled=True)
    expand_arrived = lax.all_gather(arrived, "tp", axis=1, tiled=True)
    gate = jnp.einsum("nkd,df->nkf", expand_arrived, w_gate, preferred_element_type=jnp.float32)
    upper = jnp.einsum("nkd,df->nkf", expand_arrived, w_up, preferred_element_type=jnp.float32)
    hidden = (jax.nn.silu(gate) * upper).astype(jnp.bfloat16)
    flat_hidden = hidden.reshape(-1, hidden.shape[2])
    w_down = down_weight[0]
    columns = D // lax.axis_size("tp")
    summed = lax.psum_scatter(
        lax.dot_general(
            w_down, flat_hidden, (((0,), (1,)), ((), ())), preferred_element_type=jnp.float32
        ),
        "tp",
        scatter_dimension=0,
        tiled=True,
    ).astype(jnp.bfloat16)
    back = lax.all_to_all(
        summed.reshape(columns, -1, slots), "ep", split_axis=1, concat_axis=1, tiled=True
    )
    picked = jnp.take(back.reshape(columns, experts * slots), slot_index, axis=1)
    weighted = picked.astype(jnp.float32).reshape(columns, tokens, 2) * route_weight[None, :, :]
    moe_out = jnp.sum(weighted, axis=2).T.astype(jnp.bfloat16)
    return (mixer_out, moe_out)


F32, BF16, I32 = jnp.float32, jnp.bfloat16, jnp.int32
EXTRA = 128


def exchanged(value, axes, partner):
    count = 1
    for axis in axes:
        count *= lax.axis_size(axis)
    return lax.ppermute(value, axes, [(i, partner(i)) for i in range(count)])


def swapped(value, axis):
    return exchanged(value, (axis,), lambda i: i ^ 1)


def near_by(value):
    return pltpu.with_memory_space_constraint(value, pltpu.VMEM)


def vmem():
    return pl.BlockSpec(memory_space=pltpu.VMEM)


def smem():
    return pl.BlockSpec(memory_space=pltpu.SMEM)


def room(mib):
    return pltpu.CompilerParams(vmem_limit_bytes=mib << 20)


def cost(flops):
    return pl.CostEstimate(flops=flops, bytes_accessed=0, transcendentals=0)


def dot(a, b):
    return jnp.dot(a, b, preferred_element_type=F32)


def dispatch(moe_in, moe_gain, expert_rows, weight_rows, place, cap):
    tokens, width = moe_in.shape
    half, side = cap // 2, width // 2
    groups = EXPERT_GROUPS

    def kernel(place_ref, x_ref, gain_ref, expert_ref, weight_ref, key_ref, home_ref, first_ref, *out_refs):
        z, x, c = place_ref[0], place_ref[1], place_ref[2]
        near = pl.ds(pl.multiple_of(x * side, side), side)
        far = pl.ds(pl.multiple_of((1 - x) * side, side), side)
        feats = [x_ref[:, at].astype(F32) for at in (near, far)]
        total = sum(jnp.sum(f * f, axis=1, keepdims=True) for f in feats)
        scale = lax.rsqrt(total / width + EPS)
        normed = [(f * scale * gain_ref[:, at]).astype(BF16) for f, at in zip(feats, (near, far))]
        expert = expert_ref[...]
        first = expert[0:1]
        group = lax.shift_right_logical(first, 1)
        member = (lax.broadcasted_iota(I32, (8, tokens), 0) == group).astype(F32)
        before = lax.broadcasted_iota(I32, (tokens, tokens), 0) < lax.broadcasted_iota(
            I32, (tokens, tokens), 1
        )
        earlier = dot(member.astype(BF16), before.astype(BF16))
        slot = jnp.sum(member * earlier, axis=0, keepdims=True).astype(I32)
        ahead = group ^ z
        local = slot - c * half
        mine = (local >= 0) & (local < half)
        local = jnp.where(local < 0, local + cap, local)
        key_ref[...] = jnp.broadcast_to(ahead * cap + local, (8, tokens))
        sent = jnp.where(ahead == 0, local, jnp.where(mine, half + ahead * half + local, -1))
        rows = cap + (groups - 1) * half
        pick = (lax.broadcasted_iota(I32, (rows, tokens), 0) == sent).astype(BF16)
        weight = weight_ref[...]
        even = (first & 1) == 0
        low = jnp.where(even, weight[0:1], weight[1:2])
        high = jnp.where(even, weight[1:2], weight[0:1])
        parts = []
        for w in (low, high):
            top = w.astype(BF16).astype(F32)
            parts += [top, w - top]
        lane = lax.broadcasted_iota(I32, (8, EXTRA), 1)
        row = lax.broadcasted_iota(I32, (8, EXTRA), 0)
        spread = (lane == row).astype(BF16)
        stacked = jnp.concatenate(parts + [jnp.zeros((4, tokens), F32)], axis=0).astype(BF16)
        table = lax.dot_general(
            stacked, spread, (((0,), (0,)), ((), ())), preferred_element_type=F32
        ).astype(BF16)
        own = dot(pick, normed[0]).astype(BF16)
        extra = dot(pick, table).astype(BF16)
        for d in range(1, groups):
            at = cap + (d - 1) * half
            out_refs[d - 1][:, :side] = own[at : at + half]
            out_refs[d - 1][:, side:] = extra[at : at + half]
        rest = dot(pick[:cap], normed[1]).astype(BF16)
        for ref, n in ((home_ref, cap), (first_ref, half)):
            ref[:, :side] = own[:n]
            ref[:, side:width] = rest[:n]
            ref[:, width:] = extra[:n]

    return pl.pallas_call(
        kernel,
        out_shape=[
            pltpu.VMEM((8, tokens), I32),
            pltpu.VMEM((cap, width + EXTRA), BF16),
            pltpu.VMEM((half, width + EXTRA), BF16),
        ]
        + [pltpu.VMEM((half, side + EXTRA), BF16)] * (groups - 1),
        in_specs=[smem(), vmem(), vmem(), vmem(), vmem()],
        out_specs=[vmem()] * (2 + groups),
        name="dispatch",
        compiler_params=room(20),
        cost_estimate=cost(2 << 30),
    )(place, near_by(moe_in), moe_gain.reshape(1, width), expert_rows, weight_rows)


def expand(chunks, w_gate, w_up, place):
    width, units = w_gate.shape
    side = width // 2
    half = chunks[0][2].shape[0]
    total = 4 * half * len(chunks)
    pieces = [p for chunk in chunks for p in chunk[1:]]

    def kernel(place_ref, *refs):
        gate_ref, up_ref, out_ref, x_buf, e_buf = refs[len(pieces) :]
        y, x, c = place_ref[0], place_ref[1], place_ref[2]
        at = 0
        grouped = []
        for chunk in chunks:
            grouped.append((chunk[0], refs[at : at + len(chunk) - 1]))
            at += len(chunk) - 1
        row = 0
        for far in (0, 1):
            for kind, group in grouped:
                keep, other = pl.ds(row, half), pl.ds(row + half, half)
                row += 2 * half
                if kind == "home":
                    home, near_y, far_y = group
                    rows = slice(far * half, far * half + half)
                    peer = far_y if far else near_y
                    x_buf[keep, :] = home[rows, :width]
                    e_buf[keep, :] = home[rows, width:]
                    x_buf[other, :] = peer[:, :width]
                    e_buf[other, :] = peer[:, width:]
                else:
                    own, p1, p2, p3 = group[4 * far : 4 * far + 4]
                    x_buf[keep, :side] = own[:, :side]
                    e_buf[keep, :] = own[:, side:]
                    x_buf[other, side:] = p3[:, :side]
                    e_buf[other, :] = p3[:, side:]

                    def place_both(beside, across, keep=keep, other=other):
                        x_buf[keep, side:] = beside[:, :side]
                        x_buf[other, :side] = across[:, :side]

                    @pl.when(c == far)
                    def _():
                        place_both(p2, p1)

                    @pl.when(c != far)
                    def _():
                        place_both(p1, p2)

        near_w = pl.ds(pl.multiple_of(x * side, side), side)
        far_w = pl.ds(pl.multiple_of((1 - x) * side, side), side)
        gate = dot(x_buf[:, :side], gate_ref[near_w, :]) + dot(x_buf[:, side:], gate_ref[far_w, :])
        upper = dot(x_buf[:, :side], up_ref[near_w, :]) + dot(x_buf[:, side:], up_ref[far_w, :])
        extra = e_buf[...].astype(F32)
        lane = lax.broadcasted_iota(I32, extra.shape, 1)
        wanted = lax.shift_right_logical(lane, 1) == y
        weight = jnp.sum(jnp.where(wanted, extra, 0.0), axis=1, keepdims=True)
        out_ref[...] = (gate / (1.0 + jnp.exp(-gate)) * upper * weight).astype(BF16)

    return pl.pallas_call(
        kernel,
        out_shape=pltpu.VMEM((total, units), BF16),
        in_specs=[smem()] + [vmem()] * (len(pieces) + 2),
        out_specs=vmem(),
        scratch_shapes=[pltpu.VMEM((total, width), BF16), pltpu.VMEM((total, EXTRA), BF16)],
        name="expand",
        compiler_params=room(20),
        cost_estimate=cost(4 * total * width * units),
    )(place, *map(near_by, pieces), w_gate, w_up)


def contract(own, beside, far, far_beside, w_own, w_beside, w_far, w_far_beside, place, count):
    units = own.shape[1]
    columns = w_beside.shape[1] // 2
    total = own.shape[0]
    half = total // (4 * count)

    def kernel(place_ref, o_ref, b_ref, f_ref, g_ref, wo_ref, wb_ref, wf_ref, wg_ref, *out_refs):
        x, c = place_ref[1], place_ref[2]
        whole = pl.ds(pl.multiple_of((2 * x + c) * columns, columns), columns)
        part = pl.ds(pl.multiple_of(c * columns, columns), columns)
        middle = total // 2

        def crossed(ref):
            return jnp.concatenate([ref[middle:, :], ref[:middle, :]], axis=0)

        out = dot(o_ref[...], wo_ref[:, whole])
        out = out + dot(b_ref[...], wb_ref[:, part])
        out = out + dot(crossed(f_ref), wf_ref[:, whole])
        out = out + dot(crossed(g_ref), wg_ref[:, part])
        out = out.astype(BF16)
        for i in range(count):
            for other in (0, 1):
                for far_side in (0, 1):
                    at = far_side * middle + (2 * i + other) * half
                    out_refs[2 * i + other][pl.ds(far_side * half, half), :] = out[at : at + half]

    return pl.pallas_call(
        kernel,
        out_shape=[pltpu.VMEM((2 * half, columns), BF16)] * (2 * count),
        in_specs=[smem()] + [vmem()] * 8,
        out_specs=[vmem()] * (2 * count),
        name="contract",
        compiler_params=room(16),
        cost_estimate=cost(2 * total * 4 * units * columns),
    )(
        place,
        *map(near_by, (own, beside, far, far_beside, w_own, w_beside, w_far, w_far_beside)),
    )


def restore(key, pieces):
    tokens = key.shape[1]
    cap, columns = pieces[0].shape

    def kernel(key_ref, *refs):
        out_ref = refs[-1]
        total = None
        for d, r in enumerate(refs[:-1]):
            row = lax.broadcasted_iota(I32, (cap, tokens), 0) + d * cap
            pick = (row == key_ref[0:1]).astype(BF16)
            part = lax.dot_general(
                pick, r[...], (((0,), (0,)), ((), ())), preferred_element_type=F32
            )
            total = part if total is None else total + part
        out_ref[...] = total.astype(BF16)

    return pl.pallas_call(
        kernel,
        out_shape=jax.ShapeDtypeStruct((tokens, columns), BF16),
        in_specs=[vmem()] * (1 + len(pieces)),
        out_specs=vmem(),
        name="restore",
        compiler_params=room(16),
        cost_estimate=cost(1 << 30),
    )(key, *map(near_by, pieces))


def pool(mixer_in, halo, squares, gain, weight, scale, place):
    rows, width = mixer_in.shape
    reach = WINDOW_MAX
    block = 256
    steps = rows // block

    def kernel(place_ref, x_ref, prev_ref, halo_ref, sq_ref, psq_ref, gain_ref, w_ref, s_ref, out_ref):
        i = pl.program_id(0)
        span = lax.shift_left(jnp.int32(2), place_ref[1])
        ahead = jnp.where(i == 0, halo_ref[...].astype(F32), prev_ref[...].astype(F32))
        x = jnp.concatenate([ahead, x_ref[...].astype(F32)], axis=0)
        total = jnp.concatenate([psq_ref[...], sq_ref[...]], axis=0)
        normed = (x * lax.rsqrt(total / D + EPS) * gain_ref[...]).astype(BF16)
        r = lax.broadcasted_iota(I32, (block, block + reach), 0)
        q = lax.broadcasted_iota(I32, (block, block + reach), 1)
        back = r + reach - q
        band = ((back >= 0) & (back < span)).astype(BF16)
        sums = dot(band, normed)
        position = place_ref[0] * rows + i * block + lax.broadcasted_iota(I32, (block, 1), 0)
        count = jnp.minimum(position + 1, span).astype(F32)
        pooled = (sums / count - normed[reach:].astype(F32)).astype(BF16)
        out_ref[...] = (dot(pooled, w_ref[...]) * s_ref[...]).astype(BF16)

    ratio = block // reach
    return pl.pallas_call(
        kernel,
        grid=(steps,),
        out_shape=jax.ShapeDtypeStruct((rows, width), BF16),
        in_specs=[
            smem(),
            pl.BlockSpec((block, width), lambda i: (i, 0)),
            pl.BlockSpec((reach, width), lambda i: (jnp.maximum(i * ratio - 1, 0), 0)),
            pl.BlockSpec((reach, width), lambda i: (0, 0)),
            pl.BlockSpec((block, 1), lambda i: (i, 0)),
            pl.BlockSpec((reach, 1), lambda i: (jnp.where(i == 0, steps * ratio, i * ratio - 1), 0)),
            pl.BlockSpec((1, width), lambda i: (0, 0)),
            pl.BlockSpec((width, width), lambda i: (0, 0)),
            pl.BlockSpec((1, width), lambda i: (0, 0)),
        ],
        out_specs=pl.BlockSpec((block, width), lambda i: (i, 0)),
        name="pool",
        compiler_params=room(16),
        cost_estimate=cost(2 * rows * width * (width + block + reach)),
    )(
        place,
        mixer_in,
        mixer_in,
        halo,
        squares,
        squares,
        gain.reshape(1, width),
        weight,
        scale.reshape(1, width),
    )


def paired(
    mixer_in,
    mixer_gain,
    pool_weight,
    pool_scale,
    moe_in,
    moe_gain,
    route_expert,
    route_weight,
    gate_weight,
    up_weight,
    down_weight,
):
    z, y, x, c = (lax.axis_index(a) for a in ("z", "y", "x", "c"))
    tokens = moe_in.shape[0]
    cap = 3 * tokens // (2 * EXPERT_GROUPS)
    half = cap // 2
    plane = ("y", "x", "c")

    key, home, to_y, *sends = dispatch(
        moe_in, moe_gain, route_expert.T, route_weight.T, jnp.stack([z, x, c]).astype(I32), cap
    )

    def first_hop(value):
        return exchanged(value, plane, lambda i: i ^ (2 if i & 1 else 4))

    def second_hop(value):
        return exchanged(value, plane, lambda i: i ^ (4 if i & 1 else 2))

    w_gate, w_up, w_down = (near_by(w[0]) for w in (gate_weight, up_weight, down_weight))
    arrived = {}
    for d in (3, 2, 1):
        arrived[d] = exchanged(sends[d - 1], ("z",), lambda i: i ^ d)
    from_y = swapped(to_y, "y")
    chunks = {0: ("home", home, from_y, swapped(from_y, "c"))}
    for d in (3, 2, 1):
        own = arrived[d]
        p1, p2 = first_hop(own), second_hop(own)
        near = [own, p1, p2, second_hop(p1)]
        chunks[d] = ("away", *near, *(swapped(v, "c") for v in near))

    side = down_weight.shape[2] // 2
    gone = lax.dynamic_slice_in_dim(down_weight[0], (1 - x) * side, side, 1)
    w_beside = swapped(gone, "x")
    w_far = swapped(down_weight[0], "c")
    w_far_beside = swapped(w_beside, "c")

    place = jnp.stack([y, x, c]).astype(I32)
    results = [None] * EXPERT_GROUPS
    for members in ((3, 0), (2, 1)):
        hidden = expand([chunks[d] for d in members], w_gate, w_up, place)
        beside = swapped(hidden, "x")
        far, far_beside = swapped(hidden, "c"), swapped(beside, "c")
        outs = contract(
            hidden, beside, far, far_beside, w_down, w_beside, w_far, w_far_beside, place, len(members)
        )
        for i, d in enumerate(members):
            both = outs[2 * i].astype(F32) + swapped(outs[2 * i + 1], "y").astype(F32)
            both = both.astype(BF16)
            results[d] = exchanged(both, ("z",), lambda i: i ^ d) if d else both
    moe_out = restore(key, results)

    rows = mixer_in.shape[0]
    reach = WINDOW_MAX
    halo = passed_along(mixer_in[rows - reach :], ("z", "y"), 1)
    squares = jnp.concatenate(
        [jnp.sum(jnp.square(v.astype(F32)), axis=1) for v in (mixer_in, halo)]
    )
    squares = squares + swapped(squares, "c")
    squares = squares + swapped(squares, "x")
    spot = jnp.stack([z * lax.axis_size("y") + y, 2 * x + c]).astype(I32)
    mixer_out = pool(
        mixer_in, halo, squares[:, None], mixer_gain, pool_weight[0], pool_scale, spot
    )
    return (mixer_out, moe_out)


def solution(mesh):
    ep, tp = mesh.shape["ep"], mesh.shape["tp"]
    body, over, a, b = shards, mesh, "ep", "tp"
    if ep == 2 * EXPERT_GROUPS and tp == 4:
        shape = (EXPERT_GROUPS, 2, 2, 2)
        over = Mesh(mesh.devices.reshape(shape), ("z", "y", "x", "c"))
        body, a, b = paired, ("z", "y"), ("x", "c")
    return jax.shard_map(
        body,
        mesh=over,
        in_specs=(
            P(a, b),
            P(b),
            P(b, None, None),
            P(b),
            P(a, None),
            P(),
            P(a, None),
            P(a, None),
            P(a, None, b),
            P(a, None, b),
            P(a, b, None),
        ),
        out_specs=(P(a, b), P(a, b)),
        check_vma=False,
    )
```
